32 devices in a mesh: sp: 16 (over z, y, core), tp: 2 (over x).
Axes of the slice: x: 2, y: 2, z: 4, core: 2. Of those that a mesh axis runs over, the one named last changes fastest.
Arguments:
- queries: bfloat16 [8192, 1024], P('sp', 'tp'), may hold values from -160 to 160
- keys: bfloat16 [8192, 256], P('sp', 'tp'), may hold values from -5 to 5
- values: bfloat16 [8192, 256], P('sp', 'tp'), may hold values from -6 to 6
- doc_ids: int32 [8192], P('sp'), may hold values from 0 to 7, never falling along the last dimension, each value on 1 to 2048 neighbouring positions
- sink_logit: float32 [16], P('tp'), may hold values from 1 to 6
- w_out: bfloat16 [1024, 2048], P('tp'), may hold values from -0.1875 to 0.1875
- residual: bfloat16 [8192, 2048], P(('sp', 'tp')), may hold values from -6 to 6
- ffn_gain: float32 [2048], replicated, may hold values from 0.1 to 1.9
- expert_ids: int32 [8192, 8], P(('sp', 'tp')), may hold values from 0 to 15, all different within a row; in each aligned block of 128 rows (0 to 127, 128 to 255, ...) at most 96 rows name the same one
- expert_weight: float32 [8192, 8], P(('sp', 'tp')), may hold values from 0.2 to 2
- exp_gate: bfloat16 [16, 2048, 512], P('sp'), may hold values from -0.125 to 0.125
- exp_up: bfloat16 [16, 2048, 512], P('sp'), may hold values from -0.125 to 0.125
- exp_down: bfloat16 [16, 512, 2048], P('sp'), may hold values from -0.25 to 0.25
- shared_gate: bfloat16 [2048, 512], P(None, 'tp'), may hold values from -0.125 to 0.125
- shared_up: bfloat16 [2048, 512], P(None, 'tp'), may hold values from -0.125 to 0.125
- shared_down: bfloat16 [512, 2048], P('tp'), may hold values from -0.25 to 0.25
Outputs:
- output: bfloat16 [8192, 2048], P(('sp', 'tp'))
The draws below stay inside these ranges and needn't reach their ends.
Inputs may be any that keep to these rules, and one draw needn't show every extreme that they name: `doc_ids`: never falling along the sequence; every document holds at most 2048 positions, and one holds exactly that many. `expert_ids`: each row names 8 different experts. In each aligned block of 128 rows no expert is named by more than 96 rows, and in some blocks one expert is named by exactly 96 rows.
All inputs are finite; a program needn't handle non-finite values.
Results may differ from the reference program's by a relative error of at most 0.018.
Values may be sent and summed in bfloat16 or wider, within the bound.
A program may use at most 128 MiB of HBM per device.

```python
import math
import jax
import jax.numpy as jnp
import numpy as np
from jax import lax

D = 2048
HQ = 16
KV = 4
HD = 64
WINDOW = 128
FF = 512
SFF = 512
TOP_K = 8
TOK_DEV = 512
ATTN_W = 1024
TOKENS = 8192
HALF = 128
EXPERTS = 16
CAP = 96
DOCS = 8
N_TP = 2


def drawn_pair(key):
    base_keys = jnp.clip(jax.random.normal(jax.random.fold_in(key, 101), (TOKENS, KV, HD), jnp.float32), -5.0, 5.0)
    return base_keys


def draw_keys(key, part):
    base_keys = drawn_pair(key)
    result = base_keys
    return result.reshape(TOKENS, KV * HD).astype(jnp.bfloat16)


def draw_queries(key, part):
    drawn_rows = jnp.clip(jax.random.normal(jax.random.fold_in(key, 105), (TOKENS, HQ * HD), jnp.float32), -5.0, 5.0)
    result = drawn_rows
    return result.astype(jnp.bfloat16)


def block_scale(stream_key, extent, cuts, smallest, high):
    factor_of, own = 1.0, jax.random.fold_in(stream_key, 6)
    for axis_at, parts in cuts:
        heights = jnp.exp(jax.random.uniform(jax.random.fold_in(own, axis_at), (parts,), jnp.float32, smallest / len(cuts), high / len(cuts)))
        factor_of = factor_of * jnp.repeat(heights, extent[axis_at] // parts).reshape([-1 if axis == axis_at else 1 for axis in range(len(extent))])
    return factor_of


def split_up(count, total, bound, lean):
    loads = [(1 << 20) // math.isqrt(rank ** lean) + 1 for rank in range(2, count + 1)]
    rest, given = total - bound - (count - 1), [1] * (count - 1)
    while rest > 0:
        free = [i for i in range(count - 1) if given[i] < bound]
        whole, budget = sum([loads[i] for i in free]), rest
        for i in free:
            extra = min(bound - given[i], max(1, budget * loads[i] // whole), rest)
            given[i] = given[i] + extra
            rest = rest - extra
    return np.array([bound] + given)


def uneven_parts(rng, count, total, limit, lean):
    if count == 2:
        one = jax.random.randint(rng, (), max(1, total - limit), min(limit, total - 1) + 1)
        return jnp.stack([one, total - one])
    lengths = jnp.asarray(split_up(count, total, limit, lean), jnp.int32)
    pairs = (count - 1) // 2
    source_of, receiver = lengths[1:1 + 2 * pairs:2], lengths[2:2 + 2 * pairs:2]
    slack = jnp.minimum(source_of - 1, limit - receiver)
    moved = jax.random.randint(jax.random.fold_in(rng, 1), (pairs,), 0, 1 << 20) % (slack + 1)
    lengths = lengths.at[1:1 + 2 * pairs:2].set(source_of - moved).at[2:2 + 2 * pairs:2].set(receiver + moved)
    return lengths[jax.random.permutation(jax.random.fold_in(rng, 2), count)]


def routed_block(key, own, number, rows, number_of, top, bound, lean):
    ranking = jax.random.permutation(key, number_of)
    packed, common = shares(number_of, rows * top, bound, lean, True), shares(number_of, rows * top, bound, lean, False)
    places = jnp.arange(number_of)

    def named(sizes, turn):
        used = int((sizes > 0).sum())
        fixed = max(1, used // 4)
        passed = fixed + (places - fixed + turn * (used - fixed)) % max(1, number_of - fixed)
        return jnp.zeros((number_of,), jnp.int32).at[ranking[jnp.where(places < fixed, places, passed)]].set(jnp.asarray(sizes, jnp.int32))

    sizes = jnp.where(number % 4 == 0, named(packed, number // 4), named(common, number - number // 4 - 1))
    mixed = jax.random.permutation(jax.random.fold_in(own, 3), number_of)
    donor, sink = mixed[0:number_of // 2 * 2:2], mixed[1:number_of // 2 * 2:2]
    room = jnp.minimum(sizes[donor] - 1, bound - sizes[sink]) // 2
    room = jnp.where((donor == ranking[0]) | (sink == ranking[0]) | (sizes[sink] == 0), 0, jnp.maximum(room, 0))
    passed = jax.random.randint(jax.random.fold_in(own, 4), (number_of // 2,), 0, 1 << 20) % (room + 1)
    sizes = sizes.at[donor].add(-passed).at[sink].add(passed)
    members = jnp.searchsorted(jnp.cumsum(sizes), jnp.arange(rows * top), side="right").astype(jnp.int32)
    listing = members.reshape(top, rows).T
    listing = listing[jax.random.permutation(jax.random.fold_in(own, 1), rows)]
    turn = jax.random.randint(jax.random.fold_in(own, 2), (rows, 1), 0, top)
    return jnp.take_along_axis(listing, (jnp.arange(top)[None, :] + turn) % top, axis=1)


def shares(amount, total, reach, skew, full):
    weights = [(1 << 20) // math.isqrt(grade ** skew) + 1 for grade in range(1, amount + 1)]
    largest = reach if full else min(reach, max(-(-total // amount), total * weights[0] // sum(weights)))
    least = 1 if total - largest >= amount - 1 else 0
    given, surplus = [largest] + [least] * (amount - 1), total - largest - least * (amount - 1)
    while surplus > 0:
        candidates = [i for i in range(1, amount) if given[i] < largest] or [i for i in range(1, amount) if given[i] < reach]
        pool, budget = sum([weights[i] for i in candidates]), surplus
        for i in candidates:
            more = min(reach - given[i], max(1, budget * weights[i] // pool), surplus)
            given[i] = given[i] + more
            surplus = surplus - more
    return np.array(given)


def centred(key, extent, deviation, limit, shards=(), kind=jnp.bfloat16):
    values = deviation * jax.random.normal(key, extent, jnp.float32)
    if shards:
        values = values * block_scale(key, extent, shards, -0.22, 0.18)
    return jnp.clip(values, -limit, limit).astype(kind)


def setup_inputs(seed: int = 0) -> dict:
    splits = jax.random.split(jax.random.key(seed), 17)
    queries = draw_queries(jax.random.fold_in(splits[16], 71), 0)
    keys = draw_keys(jax.random.fold_in(splits[16], 71), 0)
    values = centred(splits[2], (TOKENS, KV * HD), 1.0, 6.0, ((0, 16), (1, 2)))
    doc_ids = jnp.searchsorted(jnp.cumsum(uneven_parts(splits[3], DOCS, TOKENS, 4 * TOK_DEV, 2)), jnp.arange(TOKENS), side="right").astype(jnp.int32)
    sink_logit = jnp.clip(1.0 + 5.0 * jax.random.uniform(splits[4], (HQ,), jnp.float32) ** block_scale(splits[4], (HQ,), ((0, 2),), -0.2, 0.2), 1.0, 6.0)
    w_out = centred(splits[5], (ATTN_W, D), ATTN_W ** -0.5, 0.1875, ((0, 2),))
    residual = centred(splits[6], (TOKENS, D), 1.0, 6.0, ((0, 32),))
    ffn_gain = jnp.clip(1.0 + 0.18 * jax.random.normal(splits[7], (D,), jnp.float32), 0.1, 1.9)
    expert_ids_keys = jax.random.split(jax.random.fold_in(splits[8], 1), TOKENS // HALF)
    expert_ids_turns = jax.random.permutation(jax.random.fold_in(splits[8], 3), TOKENS // HALF)
    expert_ids = jax.vmap(lambda own, number: routed_block(jax.random.fold_in(splits[8], 2), own, number, HALF, EXPERTS, TOP_K, CAP, 2))(expert_ids_keys, expert_ids_turns).reshape((TOKENS, TOP_K))
    expert_weight = jnp.clip(jnp.exp(math.log(2.0) - 2.3025851 * jax.random.uniform(splits[9], (TOKENS, TOP_K), jnp.float32) ** block_scale(splits[9], (TOKENS, TOP_K), ((0, 32),), -0.2, 0.2)), 0.2, 2.0)
    exp_gate = centred(splits[10], (EXPERTS, D, FF), D ** -0.5, 0.125, ((0, 16),))
    exp_up = centred(splits[11], (EXPERTS, D, FF), D ** -0.5, 0.125, ((0, 16),))
    exp_down = centred(splits[12], (EXPERTS, FF, D), FF ** -0.5, 0.25, ((0, 16),))
    shared_gate = centred(splits[13], (D, SFF), D ** -0.5, 0.125, ((1, 2),))
    shared_up = centred(splits[14], (D, SFF), D ** -0.5, 0.125, ((1, 2),))
    shared_down = centred(splits[15], (SFF, D), SFF ** -0.5, 0.25, ((0, 2),))
    return dict(queries=queries, keys=keys, values=values, doc_ids=doc_ids, sink_logit=sink_logit, w_out=w_out, residual=residual, ffn_gain=ffn_gain, expert_ids=expert_ids, expert_weight=expert_weight, exp_gate=exp_gate, exp_up=exp_up, exp_down=exp_down, shared_gate=shared_gate, shared_up=shared_up, shared_down=shared_down)


norm_eps = 1e-06

def band_blocks(padded, width):
    span_count = padded.shape[0] // width - 2
    shaped = padded.reshape((span_count + 2, width) + padded.shape[1:])
    return jnp.concatenate([shaped[0:span_count:2], shaped[1:span_count + 1:2], shaped[2:span_count + 2:2], shaped[3:span_count + 3:2]], axis=1)

def reference(queries, keys, values, doc_ids, sink_logit, w_out, residual, ffn_gain, expert_ids, expert_weight, exp_gate, exp_up, exp_down, shared_gate, shared_up, shared_down):
    group_size = HQ // KV
    query_span = 2 * WINDOW
    block_count = TOKENS // query_span
    pad_rows = ((WINDOW, WINDOW), (0, 0))
    key_blocks = band_blocks(jnp.pad(keys, pad_rows), WINDOW).reshape(block_count, 4 * WINDOW, KV, HD)
    value_blocks = band_blocks(jnp.pad(values, pad_rows), WINDOW).reshape(block_count, 4 * WINDOW, KV, HD)
    marks = (doc_ids + 1).astype(jnp.int32)
    mark_blocks = band_blocks(jnp.pad(marks, (WINDOW, WINDOW)), WINDOW)
    query_blocks = queries.reshape(block_count, query_span, KV, group_size, HD)
    query_marks = marks.reshape(block_count, query_span)
    offset = jnp.arange(query_span, dtype=jnp.int32)[:, None] - jnp.arange(4 * WINDOW, dtype=jnp.int32)[None, :] + WINDOW
    near = jnp.abs(offset) <= WINDOW
    sink_term = sink_logit.astype(jnp.float32).reshape(KV, group_size)[:, :, None, None]

    def attend_block(inputs):
        query_in, key_in, value_in, key_marks, row_marks = inputs
        scores = jnp.einsum('qkgd,mkd->kgqm', query_in.astype(jnp.float32), key_in.astype(jnp.float32)) * HD ** (-0.5)
        allowed = near & (key_marks[None, :] == row_marks[:, None])
        scores = jnp.where(allowed[None, None], scores, -jnp.inf)
        row_max = jnp.maximum(lax.optimization_barrier(jnp.max(scores, axis=-1, keepdims=True)), sink_term)
        exp_scores = jnp.exp(scores - row_max)
        attn_probs = (exp_scores / (lax.optimization_barrier(jnp.sum(exp_scores, axis=-1, keepdims=True)) + jnp.exp(sink_term - row_max))).astype(jnp.bfloat16)
        result = jnp.einsum('kgqm,mkd->qkgd', attn_probs.astype(jnp.float32), value_in.astype(jnp.float32))
        return result.astype(jnp.bfloat16).reshape(query_span, HQ * HD)
    attended = lax.map(attend_block, (query_blocks, key_blocks, value_blocks, mark_blocks, query_marks)).reshape(TOKENS, HQ * HD)
    mixed = jnp.dot(attended, w_out, preferred_element_type=jnp.float32)
    resid = (residual.astype(jnp.float32) + mixed).astype(jnp.bfloat16)
    resid_f = resid.astype(jnp.float32)
    normed = (resid_f * lax.rsqrt(lax.optimization_barrier(jnp.mean(resid_f * resid_f, axis=-1, keepdims=True)) + norm_eps) * ffn_gain.astype(jnp.float32)).astype(jnp.bfloat16)
    shared_hidden = (jax.nn.silu(jnp.dot(normed, shared_gate, preferred_element_type=jnp.float32)) * jnp.dot(normed, shared_up, preferred_element_type=jnp.float32)).astype(jnp.bfloat16)
    block_units = SFF // N_TP
    shared_out = jnp.zeros((TOKENS, D), jnp.float32)
    for unit_block in range(N_TP):
        lower = unit_block * block_units
        partial_out = jnp.dot(shared_hidden[:, lower:lower + block_units], shared_down[lower:lower + block_units], preferred_element_type=jnp.float32)
        shared_out = shared_out + lax.optimization_barrier(partial_out.astype(jnp.bfloat16)).astype(jnp.float32)
    assign_count = TOKENS * TOP_K
    row_block = 512
    flat_ids = expert_ids.reshape(assign_count).astype(jnp.int32)
    order = jnp.argsort(flat_ids, stable=True).astype(jnp.int32)
    sorted_ids = flat_ids[order]
    counts = jnp.bincount(flat_ids, length=EXPERTS).astype(jnp.int32)
    starts = (jnp.cumsum(counts) - counts).astype(jnp.int32)
    padded = ((counts + row_block - 1) // row_block * row_block).astype(jnp.int32)
    ends = jnp.cumsum(padded).astype(jnp.int32)
    pad_starts = (ends - padded).astype(jnp.int32)
    dest = (pad_starts[sorted_ids] + jnp.arange(assign_count, dtype=jnp.int32) - starts[sorted_ids]).astype(jnp.int32)
    block_total = -(-assign_count // row_block) + EXPERTS
    row_source = jnp.full((block_total * row_block,), assign_count, jnp.int32).at[dest].set(order)
    block_expert = jnp.minimum(jnp.searchsorted(ends, jnp.arange(block_total, dtype=jnp.int32) * row_block, side='right'), EXPERTS - 1).astype(jnp.int32)
    flat_weight = expert_weight.reshape(assign_count).astype(jnp.float32)

    def expert_step(running, inputs):
        sources, expert_index = inputs
        live = sources < assign_count
        safe = jnp.minimum(sources, assign_count - 1)
        token_rows = (safe // TOP_K).astype(jnp.int32)
        gathered = normed[token_rows]
        hidden = (jax.nn.silu(jnp.dot(gathered, exp_gate[expert_index], preferred_element_type=jnp.float32)) * jnp.dot(gathered, exp_up[expert_index], preferred_element_type=jnp.float32)).astype(jnp.bfloat16)
        produced = jnp.dot(hidden, exp_down[expert_index], preferred_element_type=jnp.float32).astype(jnp.bfloat16)
        scale = jnp.where(live, flat_weight[safe], jnp.zeros_like(flat_weight[safe]))
        return (running.at[token_rows].add(scale[:, None] * produced.astype(jnp.float32)), None)
    routed, _ = lax.scan(expert_step, jnp.zeros((TOKENS, D), jnp.float32), (row_source.reshape(block_total, row_block), block_expert))
    return (resid.astype(jnp.float32) + shared_out + routed).astype(jnp.bfloat16)
```

```python
import math

import jax
import jax.numpy as jnp
from jax import lax
from jax.experimental import pallas as pl
from jax.experimental.pallas import tpu as pltpu
from jax.sharding import PartitionSpec as P

HD = 64
WINDOW = 128
PARTS = 2


norm_eps = 1e-06


def extended(cells, sides, width):
    for axis, dim in sides:
        count = lax.axis_size(axis)
        ends = count - 1
        head = lax.slice_in_dim(cells, 0, width, axis=dim)
        tail = lax.slice_in_dim(cells, cells.shape[dim] - width, cells.shape[dim], axis=dim)
        cells = jnp.concatenate(
            [
                lax.ppermute(tail, axis, [(i, (i + 1) % count) for i in range(ends)]),
                cells,
                lax.ppermute(head, axis, [((i + 1) % count, i) for i in range(ends)]),
            ],
            axis=dim,
        )
    return cells


def band_blocks(padded, width):
    span_count = padded.shape[0] // width - 2
    shaped = padded.reshape((span_count + 2, width) + padded.shape[1:])
    return jnp.concatenate(
        [
            shaped[0:span_count:2],
            shaped[1 : span_count + 1 : 2],
            shaped[2 : span_count + 2 : 2],
            shaped[3 : span_count + 3 : 2],
        ],
        axis=1,
    )


def attend(queries, ext_keys, ext_values, ext_marks, own_marks, sink_logit):
    tok_count = queries.shape[0]
    head_count = sink_logit.shape[0]
    key_heads = ext_keys.shape[1] // HD
    group_size = head_count // key_heads
    query_span = 2 * WINDOW
    block_count = tok_count // query_span
    query_blocks = queries.reshape(block_count, query_span, key_heads, group_size, HD)
    key_blocks = band_blocks(ext_keys, WINDOW).reshape(block_count, 4 * WINDOW, key_heads, HD)
    value_blocks = band_blocks(ext_values, WINDOW).reshape(block_count, 4 * WINDOW, key_heads, HD)
    mark_blocks = band_blocks(ext_marks, WINDOW)
    query_marks = own_marks.reshape(block_count, query_span)
    scores = jnp.einsum(
        "nqkgd,nmkd->nkgqm", query_blocks, key_blocks, preferred_element_type=jnp.float32
    ) * HD ** (-0.5)
    offset = (
        jnp.arange(query_span, dtype=jnp.int32)[:, None]
        - jnp.arange(4 * WINDOW, dtype=jnp.int32)[None, :]
        + WINDOW
    )
    allowed = (jnp.abs(offset) <= WINDOW)[None] & (
        mark_blocks[:, None, :] == query_marks[:, :, None]
    )
    scores = jnp.where(allowed[:, None, None], scores, -jnp.inf)
    sink_term = sink_logit.reshape(key_heads, group_size)[None, :, :, None, None]
    row_max = jnp.maximum(jnp.max(scores, axis=-1, keepdims=True), sink_term)
    exp_scores = jnp.exp(scores - row_max)
    attn_probs = (
        exp_scores / (jnp.sum(exp_scores, axis=-1, keepdims=True) + jnp.exp(sink_term - row_max))
    ).astype(jnp.bfloat16)
    result = jnp.einsum(
        "nkgqm,nmkd->nqkgd", attn_probs, value_blocks, preferred_element_type=jnp.float32
    )
    return result.astype(jnp.bfloat16).reshape(tok_count, head_count * HD)


def expert_kernel(rows_ref, scale_ref, gate_ref, up_ref, down_ref, side_ref, side_down_ref, out_ref):
    rows = rows_ref[...]
    gated = jnp.dot(rows, gate_ref[...], preferred_element_type=jnp.float32)
    lifted = jnp.dot(rows, up_ref[...], preferred_element_type=jnp.float32)
    hidden = (gated / (1.0 + jnp.exp(-gated)) * lifted).astype(jnp.bfloat16)
    produced = jnp.dot(hidden, down_ref[...], preferred_element_type=jnp.float32)
    side = jnp.dot(rows, side_ref[...], preferred_element_type=jnp.float32)
    width = side.shape[1] // 2
    side_gate, side_up = side[:, :width], side[:, width:]
    side_hidden = (side_gate / (1.0 + jnp.exp(-side_gate)) * side_up).astype(jnp.bfloat16)
    shared = jnp.dot(side_hidden, side_down_ref[...], preferred_element_type=jnp.float32)
    out_ref[...] = (
        scale_ref[...] * produced.astype(jnp.bfloat16).astype(jnp.float32) + shared
    ).astype(jnp.bfloat16)


def run_experts(rows, scale, gate_w, up_w, down_w, side_w, side_down):
    count, width = rows.shape
    tile = math.gcd(count, 256)
    whole = lambda w: pl.BlockSpec(w.shape, lambda i: (0, 0))
    units = gate_w.shape[1] + side_w.shape[1] // 2
    return pl.pallas_call(
        expert_kernel,
        grid=(count // tile,),
        in_specs=[
            pl.BlockSpec((tile, width), lambda i: (i, 0)),
            pl.BlockSpec((tile, 1), lambda i: (i, 0)),
            whole(gate_w),
            whole(up_w),
            whole(down_w),
            whole(side_w),
            whole(side_down),
        ],
        out_specs=pl.BlockSpec((tile, width), lambda i: (i, 0)),
        out_shape=jax.ShapeDtypeStruct((count, width), jnp.bfloat16),
        compiler_params=pltpu.CompilerParams(
            dimension_semantics=("arbitrary",), vmem_limit_bytes=48 * 1024 * 1024
        ),
        cost_estimate=pl.CostEstimate(
            flops=6 * count * width * units,
            bytes_accessed=4 * count * width + 6 * units * width,
            transcendentals=count * units,
        ),
    )(rows, scale, gate_w, up_w, down_w, side_w, side_down)


def shared_slice(shared_gate, shared_up, shared_down):
    sp_count, tp_count = lax.axis_size("sp"), lax.axis_size("tp")
    own, side = lax.axis_index("tp"), lax.axis_index("sp")
    units = shared_gate.shape[1] * tp_count // sp_count
    per_owner = sp_count // tp_count
    owner, offset = side // per_owner, (side % per_owner) * units
    held = jnp.concatenate(
        [
            lax.dynamic_slice_in_dim(shared_gate, offset, units, axis=1).T,
            lax.dynamic_slice_in_dim(shared_up, offset, units, axis=1).T,
            lax.dynamic_slice_in_dim(shared_down, offset, units, axis=0),
        ],
        axis=0,
    )
    chosen = held
    for shift in range(1, tp_count):
        came = lax.ppermute(held, "tp", [(i, (i + shift) % tp_count) for i in range(tp_count)])
        chosen = jnp.where((own - shift) % tp_count == owner, came, chosen)
    padded = -(-units // 128) * 128
    grown = [
        jnp.pad(chosen[i * units : (i + 1) * units], ((0, padded - units), (0, 0))) for i in range(3)
    ]
    return jnp.concatenate(grown[:2], axis=0).T, grown[2]


def shards(
    queries,
    keys,
    values,
    doc_ids,
    sink_logit,
    w_out,
    residual,
    ffn_gain,
    expert_ids,
    expert_weight,
    exp_gate,
    exp_up,
    exp_down,
    shared_gate,
    shared_up,
    shared_down,
):
    marks = (doc_ids + 1).astype(jnp.bfloat16)
    kv = keys.shape[1]
    joined = jnp.concatenate(
        [keys, values, jnp.broadcast_to(marks[:, None], (marks.shape[0], 128))], axis=1
    )
    extended_all = extended(joined, (("sp", 0),), WINDOW)
    ext_keys, ext_values, ext_marks = (
        extended_all[:, :kv],
        extended_all[:, kv : 2 * kv],
        extended_all[:, 2 * kv],
    )
    attended = attend(queries, ext_keys, ext_values, ext_marks, marks, sink_logit)
    row_count = residual.shape[0]
    mixed = lax.psum_scatter(
        jnp.dot(attended, w_out, preferred_element_type=jnp.float32).astype(jnp.bfloat16),
        "tp",
        scatter_dimension=0,
        tiled=True,
    ).astype(jnp.float32)
    resid = (residual.astype(jnp.float32) + mixed).astype(jnp.bfloat16)
    resid_f = resid.astype(jnp.float32)
    normed = (
        resid_f
        * lax.rsqrt(jnp.mean(resid_f * resid_f, axis=-1, keepdims=True) + norm_eps)
        * ffn_gain
    ).astype(jnp.bfloat16)
    side_w, side_down = shared_slice(shared_gate, shared_up, shared_down)
    sp_count = lax.axis_size("sp")
    chosen = expert_ids[:, :, None] == jnp.arange(sp_count, dtype=jnp.int32)
    table = jnp.sum(jnp.where(chosen, expert_weight[:, :, None], 0.0), axis=1)
    scales = lax.all_to_all(table.T, "sp", split_axis=0, concat_axis=0, tiled=True)
    part_rows = row_count // PARTS
    sums = []
    for part in range(PARTS):
        begin = part * part_rows
        gathered = lax.all_gather(normed[begin : begin + part_rows], "sp", axis=0, tiled=True)
        scale = scales[:, begin : begin + part_rows].reshape(-1, 1)
        produced = run_experts(
            gathered, scale, exp_gate[0], exp_up[0], exp_down[0], side_w, side_down
        )
        sums.append(lax.psum_scatter(produced, "sp", scatter_dimension=0, tiled=True))
    added = jnp.concatenate(sums, axis=0)
    return (resid.astype(jnp.float32) + added.astype(jnp.float32)).astype(jnp.bfloat16)


def solution(mesh):
    placed = (
        P("sp", "tp"),
        P("sp", "tp"),
        P("sp", "tp"),
        P("sp"),
        P("tp"),
        P("tp", None),
        P(("sp", "tp"), None),
        P(),
        P(("sp", "tp"), None),
        P(("sp", "tp"), None),
        P("sp", None, None),
        P("sp", None, None),
        P("sp", None, None),
        P(None, "tp"),
        P(None, "tp"),
        P("tp", None),
    )
    return jax.shard_map(
        shards, mesh=mesh, in_specs=placed, out_specs=P(("sp", "tp"), None), check_vma=False
    )
```

```python
import math

import jax
import jax.numpy as jnp
from jax import lax
from jax.experimental import pallas as pl
from jax.experimental.pallas import tpu as pltpu
from jax.sharding import PartitionSpec as P

HD = 64
WINDOW = 128
PARTS = 4
DIRECT = 2


norm_eps = 1e-06


def extended(cells, sides, width):
    for axis, dim in sides:
        count = lax.axis_size(axis)
        ends = count - 1
        head = lax.slice_in_dim(cells, 0, width, axis=dim)
        tail = lax.slice_in_dim(cells, cells.shape[dim] - width, cells.shape[dim], axis=dim)
        cells = jnp.concatenate(
            [
                lax.ppermute(tail, axis, [(i, (i + 1) % count) for i in range(ends)]),
                cells,
                lax.ppermute(head, axis, [((i + 1) % count, i) for i in range(ends)]),
            ],
            axis=dim,
        )
    return cells


def band_blocks(padded, width):
    span_count = padded.shape[0] // width - 2
    shaped = padded.reshape((span_count + 2, width) + padded.shape[1:])
    return jnp.concatenate(
        [
            shaped[0:span_count:2],
            shaped[1 : span_count + 1 : 2],
            shaped[2 : span_count + 2 : 2],
            shaped[3 : span_count + 3 : 2],
        ],
        axis=1,
    )


def attend(queries, ext_keys, ext_values, ext_marks, own_marks, sink_logit):
    tok_count = queries.shape[0]
    head_count = sink_logit.shape[0]
    key_heads = ext_keys.shape[1] // HD
    group_size = head_count // key_heads
    query_span = 2 * WINDOW
    block_count = tok_count // query_span
    query_blocks = queries.reshape(block_count, query_span, key_heads, group_size, HD)
    key_blocks = band_blocks(ext_keys, WINDOW).reshape(block_count, 4 * WINDOW, key_heads, HD)
    value_blocks = band_blocks(ext_values, WINDOW).reshape(block_count, 4 * WINDOW, key_heads, HD)
    mark_blocks = band_blocks(ext_marks, WINDOW)
    query_marks = own_marks.reshape(block_count, query_span)
    scores = jnp.einsum(
        "nqkgd,nmkd->nkgqm", query_blocks, key_blocks, preferred_element_type=jnp.float32
    ) * HD ** (-0.5)
    offset = (
        jnp.arange(query_span, dtype=jnp.int32)[:, None]
        - jnp.arange(4 * WINDOW, dtype=jnp.int32)[None, :]
        + WINDOW
    )
    allowed = (jnp.abs(offset) <= WINDOW)[None] & (
        mark_blocks[:, None, :] == query_marks[:, :, None]
    )
    scores = jnp.where(allowed[:, None, None], scores, -jnp.inf)
    sink_term = sink_logit.reshape(key_heads, group_size)[None, :, :, None, None]
    row_max = jnp.maximum(jnp.max(scores, axis=-1, keepdims=True), sink_term)
    exp_scores = jnp.exp(scores - row_max)
    attn_probs = (
        exp_scores / (jnp.sum(exp_scores, axis=-1, keepdims=True) + jnp.exp(sink_term - row_max))
    ).astype(jnp.bfloat16)
    result = jnp.einsum(
        "nkgqm,nmkd->nqkgd", attn_probs, value_blocks, preferred_element_type=jnp.float32
    )
    return result.astype(jnp.bfloat16).reshape(tok_count, head_count * HD)


def expert_kernel(rows_ref, scale_ref, gate_ref, up_ref, down_ref, side_ref, side_down_ref, out_ref):
    rows = rows_ref[...]
    gated = jnp.dot(rows, gate_ref[...], preferred_element_type=jnp.float32)
    lifted = jnp.dot(rows, up_ref[...], preferred_element_type=jnp.float32)
    hidden = (gated / (1.0 + jnp.exp(-gated)) * lifted).astype(jnp.bfloat16)
    produced = jnp.dot(hidden, down_ref[...], preferred_element_type=jnp.float32)
    side = jnp.dot(rows, side_ref[...], preferred_element_type=jnp.float32)
    width = side.shape[1] // 2
    side_gate, side_up = side[:, :width], side[:, width:]
    side_hidden = (side_gate / (1.0 + jnp.exp(-side_gate)) * side_up).astype(jnp.bfloat16)
    shared = jnp.dot(side_hidden, side_down_ref[...], preferred_element_type=jnp.float32)
    out_ref[...] = (
        scale_ref[...] * produced.astype(jnp.bfloat16).astype(jnp.float32) + shared
    ).astype(jnp.bfloat16)


def run_experts(rows, scale, gate_w, up_w, down_w, side_w, side_down):
    count, width = rows.shape
    tile = math.gcd(count, 256)
    whole = lambda w: pl.BlockSpec(w.shape, lambda i: (0, 0))
    units = gate_w.shape[1] + side_w.shape[1] // 2
    return pl.pallas_call(
        expert_kernel,
        grid=(count // tile,),
        in_specs=[
            pl.BlockSpec((tile, width), lambda i: (i, 0)),
            pl.BlockSpec((tile, 1), lambda i: (i, 0)),
            whole(gate_w),
            whole(up_w),
            whole(down_w),
            whole(side_w),
            whole(side_down),
        ],
        out_specs=pl.BlockSpec((tile, width), lambda i: (i, 0)),
        out_shape=jax.ShapeDtypeStruct((count, width), jnp.bfloat16),
        compiler_params=pltpu.CompilerParams(
            dimension_semantics=("arbitrary",), vmem_limit_bytes=48 * 1024 * 1024
        ),
        cost_estimate=pl.CostEstimate(
            flops=6 * count * width * units,
            bytes_accessed=4 * count * width + 6 * units * width,
            transcendentals=count * units,
        ),
    )(rows, scale, gate_w, up_w, down_w, side_w, side_down)


def shared_slice(shared_gate, shared_up, shared_down):
    sp_count, tp_count = lax.axis_size("sp"), lax.axis_size("tp")
    own, side = lax.axis_index("tp"), lax.axis_index("sp")
    units = shared_gate.shape[1] * tp_count // sp_count
    per_owner = sp_count // tp_count
    owner, offset = side // per_owner, (side % per_owner) * units
    held = jnp.concatenate(
        [
            lax.dynamic_slice_in_dim(shared_gate, offset, units, axis=1).T,
            lax.dynamic_slice_in_dim(shared_up, offset, units, axis=1).T,
            lax.dynamic_slice_in_dim(shared_down, offset, units, axis=0),
        ],
        axis=0,
    )
    chosen = held
    for shift in range(1, tp_count):
        came = lax.ppermute(held, "tp", [(i, (i + shift) % tp_count) for i in range(tp_count)])
        chosen = jnp.where((own - shift) % tp_count == owner, came, chosen)
    padded = -(-units // 128) * 128
    grown = [
        jnp.pad(chosen[i * units : (i + 1) * units], ((0, padded - units), (0, 0))) for i in range(3)
    ]
    return jnp.concatenate(grown[:2], axis=0).T, grown[2]


def tp_scatter(product, row_count):
    count, own = lax.axis_size("tp"), lax.axis_index("tp")
    total = lax.dynamic_slice_in_dim(product, own * row_count, row_count, axis=0)
    for shift in range(1, count):
        target = (own + shift) % count
        block = lax.dynamic_slice_in_dim(product, target * row_count, row_count, axis=0)
        came = lax.ppermute(
            block.astype(jnp.bfloat16), "tp", [(i, (i + shift) % count) for i in range(count)]
        )
        total = total + came.astype(jnp.float32)
    return total


def shards(
    queries,
    keys,
    values,
    doc_ids,
    sink_logit,
    w_out,
    residual,
    ffn_gain,
    expert_ids,
    expert_weight,
    exp_gate,
    exp_up,
    exp_down,
    shared_gate,
    shared_up,
    shared_down,
):
    marks = (doc_ids + 1).astype(jnp.bfloat16)
    kv = keys.shape[1]
    joined = jnp.concatenate(
        [keys, values, jnp.broadcast_to(marks[:, None], (marks.shape[0], 128))], axis=1
    )
    extended_all = extended(joined, (("sp", 0),), WINDOW)
    ext_keys, ext_values, ext_marks = (
        extended_all[:, :kv],
        extended_all[:, kv : 2 * kv],
        extended_all[:, 2 * kv],
    )
    attended = attend(queries, ext_keys, ext_values, ext_marks, marks, sink_logit)
    row_count = residual.shape[0]
    mixed = tp_scatter(jnp.dot(attended, w_out, preferred_element_type=jnp.float32), row_count)
    resid = (residual.astype(jnp.float32) + mixed).astype(jnp.bfloat16)
    resid_f = resid.astype(jnp.float32)
    normed = (
        resid_f
        * lax.rsqrt(jnp.mean(resid_f * resid_f, axis=-1, keepdims=True) + norm_eps)
        * ffn_gain
    ).astype(jnp.bfloat16)
    side_w, side_down = shared_slice(shared_gate, shared_up, shared_down)
    sp_count = lax.axis_size("sp")
    chosen = expert_ids[:, :, None] == jnp.arange(sp_count, dtype=jnp.int32)
    table = jnp.sum(jnp.where(chosen, expert_weight[:, :, None], 0.0), axis=1)
    scales = lax.all_to_all(table.T, "sp", split_axis=0, concat_axis=0, tiled=True)
    part_rows = row_count // PARTS
    sums = []
    for part in range(PARTS):
        begin = part * part_rows
        gathered = lax.all_gather(normed[begin : begin + part_rows], "sp", axis=0, tiled=True)
        scale = scales[:, begin : begin + part_rows].reshape(-1, 1)
        produced = run_experts(
            gathered, scale, exp_gate[0], exp_up[0], exp_down[0], side_w, side_down
        )
        if part < DIRECT:
            came = lax.all_to_all(produced, "sp", split_axis=0, concat_axis=0, tiled=True)
            came = came.reshape(sp_count, part_rows, came.shape[1])
            sums.append(jnp.sum(came.astype(jnp.float32), axis=0))
        else:
            summed = lax.psum_scatter(produced, "sp", scatter_dimension=0, tiled=True)
            sums.append(summed.astype(jnp.float32))
    added = jnp.concatenate(sums, axis=0)
    return (resid.astype(jnp.float32) + added).astype(jnp.bfloat16)


def solution(mesh):
    placed = (
        P("sp", "tp"),
        P("sp", "tp"),
        P("sp", "tp"),
        P("sp"),
        P("tp"),
        P("tp", None),
        P(("sp", "tp"), None),
        P(),
        P(("sp", "tp"), None),
        P(("sp", "tp"), None),
        P("sp", None, None),
        P("sp", None, None),
        P("sp", None, None),
        P(None, "tp"),
        P(None, "tp"),
        P("tp", None),
    )
    return jax.shard_map(
        shards, mesh=mesh, in_specs=placed, out_specs=P(("sp", "tp"), None), check_vma=False
    )
```
